32 devices in a mesh: sp: 4 (over z), tp: 4 (over y, x), dp: 2 (over core).
Axes of the slice: x: 2, y: 2, z: 4, core: 2. Of those that a mesh axis runs over, the one named last changes fastest.
Arguments:
- latent: bfloat16 [2, 1024, 2048], P('dp', 'sp'), may hold values from -1.5 to 1.5
- condition: bfloat16 [2, 2048], P('dp', 'sp'), may hold values from -6 to 6
- context: bfloat16 [2, 1024, 2048], P('dp', 'sp'), may hold values from -6 to 6
- context_code: bfloat16 [2048], P('sp'), may hold values from -6 to 6
- shift_weight: bfloat16 [2048, 2048], P('sp', 'tp'), may hold values from -0.125 to 0.125
- scale_weight: bfloat16 [2048, 2048], P('sp', 'tp'), may hold values from -0.125 to 0.125
- gate_weight: bfloat16 [2048, 2048], P('sp', 'tp'), may hold values from -0.125 to 0.125
- norm_gain: float32 [2048], replicated, may hold values from 0.1 to 1.9
- query_weight: bfloat16 [2048, 1024], P(None, 'tp'), may hold values from -0.125 to 0.125
- key_weight: bfloat16 [2048, 256], P(None, 'tp'), may hold values from -0.125 to 0.125
- value_weight: bfloat16 [2048, 256], P(None, 'tp'), may hold values from -0.125 to 0.125
- output_weight: bfloat16 [1024, 2048], P('tp'), may hold values from -0.75 to 0.75
- query_gain: float32 [64], replicated, may hold values from 1 to 5.5
- key_gain: float32 [64], replicated, may hold values from 1 to 5.5
- context_bias: float32 [16], P('tp'), may hold values from 0.5 to 2
Outputs:
- updated: bfloat16 [2, 1024, 2048], P('dp', 'sp')
The draws below stay inside these ranges and needn't reach their ends.
All inputs are finite; a program needn't handle non-finite values.
Results may differ from the reference program's by a relative error of at most 0.01405.
The reference program's roundings to bfloat16 on the way count: a program that leaves them out, or rounds other values in their place, can miss the bound.
Values may be sent and summed in bfloat16 or wider, within the bound.
No kernel may reach another device: no remote copies, remote signals or barrier semaphores. Data moves between devices by JAX's collectives and lax.ppermute only.
A program may use at most 64 MiB of HBM per device.

```python
import math
import jax
import jax.numpy as jnp
from jax import lax

D = 2048
HEADS = 16
KV_HEADS = 4
HEAD = 64
GRID_W = 64
CTX = 1024
SAMPLES = 2
SEQ = 1024


def gain_draw(key, salt):
    fresh = jax.random.fold_in(key, salt)
    return jnp.exp(jax.random.uniform(fresh, (HEAD,), jnp.float32, 0.0, math.log(2.2)))


def draw_query_gain(key, part):
    return gain_draw(key, 17)


def draw_key_gain(key, part):
    return gain_draw(key, 29)


def shard_levels(rng, dims, cuts, smallest, largest):
    gain, own = 1.0, jax.random.fold_in(rng, 6)
    for dim, blocks in cuts:
        draws = jnp.exp(jax.random.uniform(jax.random.fold_in(own, dim), (blocks,), jnp.float32, smallest / len(cuts), largest / len(cuts)))
        gain = gain * jnp.repeat(draws, dims[dim] // blocks).reshape([-1 if axis == dim else 1 for axis in range(len(dims))])
    return gain


def centred(stream_key, dims, spread, bound, split=(), kind=jnp.bfloat16):
    entries = spread * jax.random.normal(stream_key, dims, jnp.float32)
    if split:
        entries = entries * shard_levels(stream_key, dims, split, -0.22, 0.18)
    return jnp.clip(entries, -bound, bound).astype(kind)


def setup_inputs(seed: int = 0) -> dict:
    key_of = jax.random.split(jax.random.key(seed), 16)
    latent = centred(key_of[0], (SAMPLES, SEQ, D), 0.25, 1.5, ((0, 2), (1, 4)))
    condition = centred(key_of[1], (SAMPLES, D), 1.0, 6.0, ((0, 2), (1, 4)))
    context = centred(key_of[2], (SAMPLES, CTX, D), 1.0, 6.0, ((0, 2), (1, 4)))
    context_code = centred(key_of[3], (D,), 1.0, 6.0, ((0, 4),))
    shift_weight = centred(key_of[4], (D, D), D ** -0.5, 0.125, ((0, 4), (1, 4)))
    scale_weight = centred(key_of[5], (D, D), D ** -0.5, 0.125, ((0, 4), (1, 4)))
    gate_weight = centred(key_of[6], (D, D), D ** -0.5, 0.125, ((0, 4), (1, 4)))
    norm_gain = jnp.clip(1.0 + 0.18 * jax.random.normal(key_of[7], (D,), jnp.float32), 0.1, 1.9)
    query_weight = centred(key_of[8], (D, HEADS * HEAD), D ** -0.5, 0.125, ((1, 4),))
    key_weight = centred(key_of[9], (D, KV_HEADS * HEAD), D ** -0.5, 0.125, ((1, 4),))
    value_weight = centred(key_of[10], (D, KV_HEADS * HEAD), D ** -0.5, 0.125, ((1, 4),))
    output_weight = centred(key_of[11], (HEADS * HEAD, D), (HEADS * HEAD // 16) ** -0.5, 0.75, ((0, 4),))
    query_gain = draw_query_gain(jax.random.fold_in(key_of[15], 71), 0)
    key_gain = draw_key_gain(jax.random.fold_in(key_of[15], 71), 0)
    context_bias = jnp.clip(0.5 + 1.5 * jax.random.uniform(key_of[14], (HEADS,), jnp.float32) ** shard_levels(key_of[14], (HEADS,), ((0, 4),), -0.2, 0.2), 0.5, 2.0)
    return {"latent": latent, "condition": condition, "context": context, "context_code": context_code, "shift_weight": shift_weight, "scale_weight": scale_weight, "gate_weight": gate_weight, "norm_gain": norm_gain, "query_weight": query_weight, "key_weight": key_weight, "value_weight": value_weight, "output_weight": output_weight, "query_gain": query_gain, "key_gain": key_gain, "context_bias": context_bias}


norm_eps = 1e-06
rope_base = 10000.0

def rotary_tables(position):
    grid_row = (position // GRID_W).astype(jnp.float32)
    grid_col = (position % GRID_W).astype(jnp.float32)
    quarter = HEAD // 4
    inverse = rope_base ** (-jnp.arange(quarter, dtype=jnp.float32) / quarter)
    angles = jnp.concatenate([grid_row[:, None] * inverse, grid_col[:, None] * inverse], axis=-1)
    return (jnp.cos(angles), jnp.sin(angles))

def head_norm(values, gain_row):
    return values * lax.rsqrt(lax.optimization_barrier(jnp.mean(values * values, axis=-1, keepdims=True)) + norm_eps) * gain_row

def rotate(values, cosine, sine_part):
    half_dim = values.shape[-1] // 2
    first_half = values[..., :half_dim]
    second_half = values[..., half_dim:]
    cos_rows = cosine[:, None, :]
    sin_rows = sine_part[:, None, :]
    return jnp.concatenate([first_half * cos_rows - second_half * sin_rows, second_half * cos_rows + first_half * sin_rows], axis=-1)

def modulated(tokens, gain_row, shift_row, scale_row):
    floats = tokens.astype(jnp.float32)
    normal = floats * lax.rsqrt(lax.optimization_barrier(jnp.mean(floats * floats, axis=-1, keepdims=True)) + norm_eps)
    return (normal * gain_row * (1.0 + scale_row) + shift_row).astype(jnp.bfloat16)

def attend(query_block, latent_keys, latent_values, context_keys, context_values, bias_value):
    score_scale = HEAD ** (-0.5)
    latent_scores = jnp.dot(query_block, latent_keys.T, preferred_element_type=jnp.float32) * score_scale
    context_scores = jnp.dot(query_block, context_keys.T, preferred_element_type=jnp.float32) * score_scale + bias_value
    row_max = jnp.maximum(latent_scores.max(axis=1), context_scores.max(axis=1))[:, None]
    latent_exp = jnp.exp(latent_scores - row_max)
    context_exp = jnp.exp(context_scores - row_max)
    totals = latent_exp.sum(axis=1) + context_exp.sum(axis=1)
    summed = jnp.dot(latent_exp.astype(jnp.bfloat16), latent_values, preferred_element_type=jnp.float32)
    summed = summed + jnp.dot(context_exp.astype(jnp.bfloat16), context_values, preferred_element_type=jnp.float32)
    return (summed / totals[:, None]).astype(jnp.bfloat16)

def reference(latent, condition, context, context_code, shift_weight, scale_weight, gate_weight, norm_gain, query_weight, key_weight, value_weight, output_weight, query_gain, key_gain, context_bias):
    cosine, sine_part = rotary_tables(jnp.arange(SEQ, dtype=jnp.int32))
    group_size = HEADS // KV_HEADS
    query_block = math.gcd(SEQ, 512)
    context_act = jax.nn.silu(context_code.astype(jnp.float32)).astype(jnp.bfloat16)
    context_shift = jnp.dot(context_act, shift_weight, preferred_element_type=jnp.float32)
    context_scale = jnp.dot(context_act, scale_weight, preferred_element_type=jnp.float32)
    results = []
    for sample in range(SAMPLES):
        activated = jax.nn.silu(condition[sample].astype(jnp.float32)).astype(jnp.bfloat16)
        latent_shift = jnp.dot(activated, shift_weight, preferred_element_type=jnp.float32)
        latent_scale = jnp.dot(activated, scale_weight, preferred_element_type=jnp.float32)
        latent_gate = jnp.dot(activated, gate_weight, preferred_element_type=jnp.float32)
        normed = modulated(latent[sample], norm_gain, latent_shift, latent_scale)
        queries = jnp.dot(normed, query_weight, preferred_element_type=jnp.float32).reshape(SEQ, HEADS, HEAD)
        queries = rotate(head_norm(queries, query_gain), cosine, sine_part).astype(jnp.bfloat16)
        latent_keys = jnp.dot(normed, key_weight, preferred_element_type=jnp.float32).reshape(SEQ, KV_HEADS, HEAD)
        latent_keys = rotate(head_norm(latent_keys, key_gain), cosine, sine_part).astype(jnp.bfloat16)
        latent_values = jnp.dot(normed, value_weight, preferred_element_type=jnp.float32)
        latent_values = latent_values.reshape(SEQ, KV_HEADS, HEAD).astype(jnp.bfloat16)
        context_normed = modulated(context[sample], norm_gain, context_shift, context_scale)
        context_keys = jnp.dot(context_normed, key_weight, preferred_element_type=jnp.float32).reshape(CTX, KV_HEADS, HEAD)
        context_keys = head_norm(context_keys, key_gain).astype(jnp.bfloat16)
        context_values = jnp.dot(context_normed, value_weight, preferred_element_type=jnp.float32)
        context_values = context_values.reshape(CTX, KV_HEADS, HEAD).astype(jnp.bfloat16)
        mixed = jnp.zeros((SEQ, D), jnp.float32)
        for kv_head in range(KV_HEADS):
            outputs = []
            for head_index in range(kv_head * group_size, (kv_head + 1) * group_size):
                head_out = lax.map(partial_attend(latent_keys[:, kv_head], latent_values[:, kv_head], context_keys[:, kv_head], context_values[:, kv_head], context_bias[head_index]), queries[:, head_index].reshape(SEQ // query_block, query_block, HEAD))
                outputs.append(head_out.reshape(SEQ, HEAD))
            attended = jnp.concatenate(outputs, axis=1)
            rows_start = kv_head * group_size * HEAD
            weight_rows = output_weight[rows_start:rows_start + group_size * HEAD]
            partial_sum = jnp.dot(attended, weight_rows, preferred_element_type=jnp.float32).astype(jnp.bfloat16)
            mixed = mixed + partial_sum.astype(jnp.float32)
        updated = latent[sample].astype(jnp.float32) + latent_gate * mixed
        results.append(updated.astype(jnp.bfloat16))
    return jnp.stack(results)

def partial_attend(latent_keys, latent_values, context_keys, context_values, bias_value):

    def attend_block(query_block):
        return attend(query_block, latent_keys, latent_values, context_keys, context_values, bias_value)
    return attend_block
```

```python
import math

import jax
import jax.numpy as jnp
from jax import lax
from jax.sharding import PartitionSpec as P

GRID_W = 64
DIRECT_LIMIT = 4

norm_eps = 1e-06
rope_base = 10000.0


def rotary_tables(position, grid_width, head_dim):
    grid_row = (position // grid_width).astype(jnp.float32)
    grid_col = (position % grid_width).astype(jnp.float32)
    quarter = head_dim // 4
    inverse = rope_base ** (-jnp.arange(quarter, dtype=jnp.float32) / quarter)
    angles = jnp.concatenate([grid_row[:, None] * inverse, grid_col[:, None] * inverse], axis=-1)
    return (jnp.cos(angles), jnp.sin(angles))


def head_norm(values, gain_row):
    return (
        values * lax.rsqrt(jnp.mean(values * values, axis=-1, keepdims=True) + norm_eps) * gain_row
    )


def rotate(values, cosine, sine_part):
    half_dim = values.shape[-1] // 2
    first_half = values[..., :half_dim]
    second_half = values[..., half_dim:]
    cos_rows = cosine[:, None, :]
    sin_rows = sine_part[:, None, :]
    return jnp.concatenate(
        [
            first_half * cos_rows - second_half * sin_rows,
            second_half * cos_rows + first_half * sin_rows,
        ],
        axis=-1,
    )


def modulated(tokens, gain_row, shift_row, scale_row):
    floats = tokens.astype(jnp.float32)
    normal = floats * lax.rsqrt(jnp.mean(floats * floats, axis=-1, keepdims=True) + norm_eps)
    return (normal * gain_row * (1.0 + scale_row) + shift_row).astype(jnp.bfloat16)


def direct(size):
    return size <= DIRECT_LIMIT and size & (size - 1) == 0


def swap(values, axis, mask):
    size = lax.axis_size(axis)
    return lax.ppermute(values, axis, [(i, i ^ mask) for i in range(size)])


def exchange(values, axis):
    size = lax.axis_size(axis)
    got = {mask: swap(values, axis, mask) for mask in reversed(range(1, size))}
    return [values] + [got[mask] for mask in range(1, size)]


def paired_sum(parts):
    while len(parts) > 1:
        parts = [parts[i] + parts[i + 1] for i in range(0, len(parts), 2)]
    return parts[0]


def sum_over(values, axis):
    if not direct(lax.axis_size(axis)):
        return lax.psum(values, axis)
    return paired_sum(exchange(values, axis))


def columns_over(values, axis):
    size = lax.axis_size(axis)
    if not direct(size):
        return lax.all_gather(values, axis, axis=1, tiled=True)
    me = lax.axis_index(axis)
    parts = exchange(values, axis)
    blocks = []
    for block in range(size):
        chosen = parts[0]
        for mask in range(1, size):
            chosen = jnp.where(me ^ mask == block, parts[mask], chosen)
        blocks.append(chosen)
    return jnp.concatenate(blocks, axis=1)


def rows_over(values, axis):
    if not direct(lax.axis_size(axis)):
        return lax.all_gather(values, axis, axis=0, tiled=True)
    return jnp.concatenate(exchange(values, axis), axis=0)


def on_device(
    latent,
    condition,
    context,
    context_code,
    shift_weight,
    scale_weight,
    gate_weight,
    norm_gain,
    query_weight,
    key_weight,
    value_weight,
    output_weight,
    query_gain,
    key_gain,
    context_bias,
):
    head_dim = query_gain.shape[0]
    tp_size = lax.axis_size("tp")
    dp_size = lax.axis_size("dp")
    activated = jax.nn.silu(condition[0].astype(jnp.float32)).astype(jnp.bfloat16)
    context_act = jax.nn.silu(context_code.astype(jnp.float32)).astype(jnp.bfloat16)
    both = jnp.stack([activated, context_act])
    shifts = jnp.dot(both, shift_weight, preferred_element_type=jnp.float32)
    scales = jnp.dot(both, scale_weight, preferred_element_type=jnp.float32)
    gates = jnp.dot(both, gate_weight, preferred_element_type=jnp.float32)
    partial_mod = jnp.concatenate([shifts, scales, gates[:1]])

    share_cores = tp_size == 4 and dp_size == 2
    if share_cores:
        half = output_weight.shape[0] // 2
        core = lax.axis_index("dp")
        own_half = lax.dynamic_slice_in_dim(output_weight, core * half, half, 0)
        top, bottom = own_half[: half // 2], own_half[half // 2 :]
        top_x = swap(top, "tp", 1)
        bottom_y = swap(bottom, "tp", 2)

    summed = sum_over(partial_mod, "sp")
    vectors = columns_over(summed, "tp")

    if share_cores:
        top, bottom, top_x, bottom_y, vectors = lax.optimization_barrier(
            (top, bottom, top_x, bottom_y, vectors)
        )
        top_pair = swap(jnp.concatenate([top, top_x]), "tp", 2)
        bottom_pair = swap(jnp.concatenate([bottom, bottom_y]), "tp", 1)
        quarter = half // 2
        mine = jnp.stack(
            [
                jnp.concatenate([top_x, bottom_pair[:quarter]]),
                jnp.concatenate([top_pair[:quarter], bottom_y]),
                jnp.concatenate([top_pair[quarter:], bottom_pair[quarter:]]),
            ]
        )
        theirs = swap(mine, "dp", 1)

    normed = modulated(latent[0], norm_gain, vectors[0], vectors[2])
    context_normed = modulated(context[0], norm_gain, vectors[1], vectors[3])
    query_cols = query_weight.shape[1]
    seq_rows = normed.shape[0]
    position = lax.axis_index("sp") * seq_rows + jnp.arange(seq_rows, dtype=jnp.int32)
    cosine, sine_part = rotary_tables(position, GRID_W, head_dim)
    group_size = query_cols // head_dim

    context_keys = head_norm(
        jnp.dot(context_normed, key_weight, preferred_element_type=jnp.float32), key_gain
    )
    context_values = jnp.dot(context_normed, value_weight, preferred_element_type=jnp.float32)
    latent_keys = jnp.dot(normed, key_weight, preferred_element_type=jnp.float32)
    latent_keys = rotate(
        head_norm(latent_keys.reshape(seq_rows, 1, head_dim), key_gain), cosine, sine_part
    ).reshape(seq_rows, head_dim)
    latent_values = jnp.dot(normed, value_weight, preferred_element_type=jnp.float32)
    key_value = jnp.concatenate([latent_keys, latent_values], axis=1).astype(jnp.bfloat16)
    context_kv = jnp.concatenate([context_keys, context_values], axis=1).astype(jnp.bfloat16)
    ctx_rows = context_kv.shape[0]

    own_kv = jnp.concatenate([context_kv, key_value], axis=0)
    if direct(lax.axis_size("sp")):
        pieces = exchange(own_kv, "sp")
        contexts = jnp.concatenate([piece[:ctx_rows] for piece in pieces], axis=0)
        arrived = jnp.concatenate([piece[ctx_rows:] for piece in pieces], axis=0)
    else:
        contexts = rows_over(context_kv, "sp")
        arrived = rows_over(key_value, "sp")

    queries = jnp.dot(normed, query_weight, preferred_element_type=jnp.float32)
    queries = queries.reshape(seq_rows, group_size, head_dim)
    queries = rotate(head_norm(queries, query_gain), cosine, sine_part).astype(jnp.bfloat16)

    score_scale = head_dim ** (-0.5)
    query_rows = queries.transpose(1, 0, 2).reshape(group_size * seq_rows, head_dim)
    bias_rows = jnp.repeat(context_bias, seq_rows)
    context_scores = jnp.dot(
        query_rows, contexts[:, :head_dim].T, preferred_element_type=jnp.float32
    )
    context_scores = context_scores * score_scale + bias_rows[:, None]
    first_max = context_scores.max(axis=1)
    context_exp = jnp.exp(context_scores - first_max[:, None])
    start_state = (
        first_max,
        context_exp.sum(axis=1),
        jnp.dot(
            context_exp.astype(jnp.bfloat16),
            contexts[:, head_dim:],
            preferred_element_type=jnp.float32,
        ),
    )
    arrived_rows = arrived.shape[0]
    block_rows = math.gcd(arrived_rows, 1024)
    blocks = arrived.reshape(arrived_rows // block_rows, block_rows, 2 * head_dim)

    def absorb_block(state_now, pair_block):
        old_max, old_total, old_accum = state_now
        scores = (
            jnp.dot(query_rows, pair_block[:, :head_dim].T, preferred_element_type=jnp.float32)
            * score_scale
        )
        new_max = jnp.maximum(old_max, scores.max(axis=1))
        factor = jnp.exp(old_max - new_max)
        weights = jnp.exp(scores - new_max[:, None])
        new_accum = old_accum * factor[:, None] + jnp.dot(
            weights.astype(jnp.bfloat16),
            pair_block[:, head_dim:],
            preferred_element_type=jnp.float32,
        )
        return ((new_max, old_total * factor + weights.sum(axis=1), new_accum), None)

    final_state, unused = lax.scan(absorb_block, start_state, blocks)
    row_max, totals, accum = final_state
    attended = (accum / totals[:, None]).astype(jnp.bfloat16)
    attended = (
        attended.reshape(group_size, seq_rows, head_dim)
        .transpose(1, 0, 2)
        .reshape(seq_rows, query_cols)
    )

    if share_cores:
        heads_of = exchange(attended, "tp")
        partials = []
        for mask in range(tp_size):
            if mask == 0:
                rows = output_weight
            else:
                first = jnp.where(core == 0, mine[mask - 1], theirs[mask - 1])
                second = jnp.where(core == 0, theirs[mask - 1], mine[mask - 1])
                rows = jnp.concatenate([first, second])
            part = jnp.dot(heads_of[mask], rows, preferred_element_type=jnp.float32)
            partials.append(part.astype(jnp.bfloat16).astype(jnp.float32))
        mixed = paired_sum(partials)
        updated = (latent[0].astype(jnp.float32) + vectors[4] * mixed).astype(jnp.bfloat16)
        return updated[None]

    own_rows = seq_rows // tp_size
    mixed = lax.psum_scatter(
        jnp.dot(attended, output_weight, preferred_element_type=jnp.float32).astype(jnp.bfloat16),
        "tp",
        scatter_dimension=0,
        tiled=True,
    ).astype(jnp.float32)
    own_latent = lax.dynamic_slice_in_dim(latent[0], lax.axis_index("tp") * own_rows, own_rows, 0)
    updated = (own_latent.astype(jnp.float32) + vectors[4] * mixed).astype(jnp.bfloat16)
    whole = lax.all_gather(updated, "tp", axis=0, tiled=True)
    return whole[None]


def solution(mesh):
    return jax.shard_map(
        on_device,
        mesh=mesh,
        in_specs=(
            P("dp", "sp", None),
            P("dp", "sp"),
            P("dp", "sp", None),
            P("sp"),
            P("sp", "tp"),
            P("sp", "tp"),
            P("sp", "tp"),
            P(),
            P(None, "tp"),
            P(None, "tp"),
            P(None, "tp"),
            P("tp", None),
            P(),
            P(),
            P("tp"),
        ),
        out_specs=P("dp", "sp", None),
        check_vma=False,
    )
```

```python
import functools
import math

import jax
import jax.numpy as jnp
from jax import lax
from jax.experimental import pallas as pl
from jax.experimental.pallas import tpu as pltpu
from jax.sharding import PartitionSpec as P


GRID_W = 64
DIRECT_LIMIT = 4
KERNEL_VMEM = 20 << 20

norm_eps = 1e-06
rope_base = 10000.0

VMEM = pl.BlockSpec(memory_space=pltpu.VMEM)
SMEM = pl.BlockSpec(memory_space=pltpu.SMEM)
HBM = pl.BlockSpec(memory_space=pltpu.HBM)


def dot(left, right):
    return jnp.dot(left, right, preferred_element_type=jnp.float32)


def dot_t(left, right):
    return lax.dot_general(
        left, right, (((1,), (1,)), ((), ())), preferred_element_type=jnp.float32
    )


def call(kernel, outs, specs, flops, *args, **kwargs):
    return pl.pallas_call(
        kernel,
        out_shape=outs,
        in_specs=specs,
        out_specs=jax.tree.map(lambda _: VMEM, outs),
        cost_estimate=pl.CostEstimate(flops=flops, bytes_accessed=0, transcendentals=0),
        compiler_params=pltpu.CompilerParams(vmem_limit_bytes=KERNEL_VMEM),
        **kwargs,
    )(*args)


def modulation_kernel(*refs):
    sources, out_ref, buffers, semaphores = refs[:5], refs[5], refs[6:11], refs[11]
    copies = [
        pltpu.make_async_copy(source, buffer, semaphores.at[i])
        for i, (source, buffer) in enumerate(zip(sources, buffers))
    ]
    for copy in copies:
        copy.start()
    copies[0].wait()
    copies[1].wait()
    row = lax.broadcasted_iota(jnp.int32, (16, buffers[0].shape[1]), 0)
    rows = jnp.where(row == 0, buffers[0][...].astype(jnp.float32), 0.0)
    rows = jnp.where(row == 1, buffers[1][...].astype(jnp.float32)[None], rows)
    rows = (rows / (1.0 + jnp.exp(-rows))).astype(jnp.bfloat16)
    for i, copy in enumerate(copies[2:]):
        copy.wait()
        out_ref[2 * i : 2 * i + 2, :] = dot(rows, buffers[2 + i][...])[:2]


def normal_kernel(context_hbm, latent_hbm, context_ref, latent_ref, context_out, latent_out, semaphores):
    steps = []
    for source, buffer, out_ref in (
        (context_hbm, context_ref, context_out),
        (latent_hbm, latent_ref, latent_out),
    ):
        block = math.gcd(source.shape[0], 64)
        for start in range(0, source.shape[0], block):
            part = pl.ds(start, block)
            copy = pltpu.make_async_copy(
                source.at[part], buffer.at[part], semaphores.at[len(steps)]
            )
            steps.append((copy, buffer, out_ref, part))
    for copy, _, _, _ in steps:
        copy.start()
    for copy, buffer, out_ref, part in steps:
        copy.wait()
        floats = buffer[part].astype(jnp.float32)
        mean = jnp.mean(floats * floats, axis=-1, keepdims=True)
        out_ref[part] = lax.rsqrt(mean + norm_eps)


def head_norm(values, gain_row):
    mean = jnp.mean(values * values, axis=-1, keepdims=True)
    return values * lax.rsqrt(mean + norm_eps) * gain_row


def rotate(values, cosine, sine_part):
    half_dim = values.shape[-1] // 2
    turned = jnp.concatenate([-values[:, half_dim:], values[:, :half_dim]], axis=1)
    return values * cosine + turned * sine_part


def key_value_kernel(
    index_ref,
    pieces_ref,
    latent_ref,
    context_ref,
    latent_factor_ref,
    context_factor_ref,
    norm_gain_ref,
    key_w_ref,
    value_w_ref,
    gain_ref,
    cos_ref,
    sin_ref,
    kv_ref,
    normed_ref,
    gate_ref,
    rows_ref,
):
    me = index_ref[0]
    count = pieces_ref.shape[0]
    width = pieces_ref.shape[2]
    for mask in range(count):
        start = pl.multiple_of((me ^ mask) * width, width)
        rows_ref[:, pl.ds(start, width)] = pieces_ref[mask]
    ctx_rows = context_ref.shape[0]
    for is_latent, in_ref, factor_ref in (
        (False, context_ref, context_factor_ref),
        (True, latent_ref, latent_factor_ref),
    ):
        row = 0 if is_latent else 1
        shift, scale = rows_ref[row : row + 1, :], rows_ref[row + 2 : row + 3, :]
        scale = norm_gain_ref[...] * (1.0 + scale)
        normed = in_ref[...].astype(jnp.float32) * factor_ref[...]
        normed = (normed * scale + shift).astype(jnp.bfloat16)
        keys = head_norm(dot_t(normed, key_w_ref[...]), gain_ref[...])
        if is_latent:
            normed_ref[...] = normed
            keys = rotate(keys, cos_ref[...], sin_ref[...])
        values = dot_t(normed, value_w_ref[...])
        part = slice(ctx_rows, None) if is_latent else slice(0, ctx_rows)
        kv_ref[part, :] = jnp.concatenate([keys, values], axis=1).astype(jnp.bfloat16)
    gate_ref[...] = rows_ref[4:5, :]


def query_kernel(scale, normed_ref, weight_ref, gain_ref, cos_ref, sin_ref, out_ref):
    all_heads = dot(normed_ref[...], weight_ref[...])
    head_dim = gain_ref.shape[1]
    rows = all_heads.shape[0]
    for head in range(all_heads.shape[1] // head_dim):
        values = all_heads[:, head * head_dim : (head + 1) * head_dim]
        values = rotate(head_norm(values, gain_ref[...]), cos_ref[...], sin_ref[...])
        values = values.astype(jnp.bfloat16) * scale
        out_ref[head * rows : (head + 1) * rows, :] = jnp.concatenate(
            [values, jnp.zeros_like(values)], axis=1
        ).astype(jnp.bfloat16)


def with_ones(pairs):
    lane = lax.broadcasted_iota(jnp.int32, pairs.shape, 1)
    return jnp.where(lane < pairs.shape[1] // 2, jnp.ones_like(pairs), pairs)


def block_scores(queries, pair_refs, bias, ctx_rows):
    context = [dot_t(queries, ref[:ctx_rows, :]) for ref in pair_refs]
    latent = [dot_t(queries, ref[ctx_rows:, :]) for ref in pair_refs]
    tops = [functools.reduce(jnp.maximum, kind).max(axis=1, keepdims=True) for kind in (context, latent)]
    return context, latent, jnp.maximum(tops[0] + bias, tops[1])


def weigh(context, latent, top, bias, pair_refs, ctx_rows):
    weights = [jnp.exp(values - (top - bias)).astype(jnp.bfloat16) for values in context]
    weights += [jnp.exp(values - top).astype(jnp.bfloat16) for values in latent]
    pairs = [ref[:ctx_rows, :] for ref in pair_refs] + [ref[ctx_rows:, :] for ref in pair_refs]
    pairs = with_ones(jnp.concatenate(pairs, axis=0))
    return dot(jnp.concatenate(weights, axis=1), pairs)


def attend_own_kernel(ctx_rows, bias_ref, query_ref, *refs):
    pair_refs, (top_ref, sum_ref) = refs[:-2], refs[-2:]
    heads = bias_ref.shape[0]
    rows = query_ref.shape[0] // heads
    for head in range(heads):
        part = slice(head * rows, (head + 1) * rows)
        bias = bias_ref[head]
        context, latent, top = block_scores(query_ref[part, :], pair_refs, bias, ctx_rows)
        top_ref[part, :] = top
        sum_ref[part, :] = weigh(context, latent, top, bias, pair_refs, ctx_rows)


def attend_rest_kernel(ctx_rows, bias_ref, query_ref, top_ref, sum_ref, *refs):
    pair_refs, out_ref = refs[:-1], refs[-1]
    heads = bias_ref.shape[0]
    rows = query_ref.shape[0] // heads
    head_dim = query_ref.shape[1] // 2
    for head in range(heads):
        part = slice(head * rows, (head + 1) * rows)
        bias = bias_ref[head]
        context, latent, top = block_scores(query_ref[part, :], pair_refs, bias, ctx_rows)
        old_top = top_ref[part, :]
        top = jnp.maximum(top, old_top)
        total = sum_ref[part, :] * jnp.exp(old_top - top)
        total = total + weigh(context, latent, top, bias, pair_refs, ctx_rows)
        out_ref[:, head * head_dim : (head + 1) * head_dim] = (
            total[:, head_dim:] / total[:, :head_dim]
        ).astype(jnp.bfloat16)


def own_partial_kernel(heads_ref, weight_ref, out_ref):
    out_ref[...] = dot(heads_ref[...], weight_ref[...]).astype(jnp.bfloat16)


def output_kernel(
    index_ref, own_ref, one_ref, two_ref, three_ref, latent_ref, gate_ref, *refs
):
    weight_refs, out_ref = refs[:-1], refs[-1]
    width = out_ref.shape[1]
    columns = pl.ds(pl.multiple_of(pl.program_id(0) * width, width), width)
    core = index_ref[1]

    def project(x_ref, y_ref, first_ref, second_ref):
        diagonal = jnp.concatenate([first_ref[:, columns], second_ref[:, columns]], axis=0)
        parts = [
            dot(heads_ref[...], rows).astype(jnp.bfloat16).astype(jnp.float32)
            for heads_ref, rows in (
                (one_ref, x_ref[:, columns]),
                (two_ref, y_ref[:, columns]),
                (three_ref, diagonal),
            )
        ]
        mixed = (own_ref[:, columns].astype(jnp.float32) + parts[0]) + (parts[1] + parts[2])
        out_ref[...] = (
            latent_ref[:, columns].astype(jnp.float32) + gate_ref[:, columns] * mixed
        ).astype(jnp.bfloat16)

    near_ref, far_ref, other_near_ref, other_far_ref = weight_refs

    @pl.when(core == 0)
    def _():
        project(near_ref, other_near_ref, far_ref, other_far_ref)

    @pl.when(core != 0)
    def _():
        project(other_near_ref, near_ref, other_far_ref, far_ref)


def direct(size):
    return size <= DIRECT_LIMIT and size & (size - 1) == 0


def swap(values, axis, mask):
    size = lax.axis_size(axis)
    return lax.ppermute(values, axis, [(i, i ^ mask) for i in range(size)])


def core_swap(values, axis, masks):
    size, cores = lax.axis_size(axis), len(masks)
    pairs = [
        (i * cores + core, (i ^ mask) * cores + core)
        for i in range(size)
        for core, mask in enumerate(masks)
    ]
    return lax.ppermute(values, (axis, "dp"), pairs)


def exchange(values, axis):
    masks = range(1, lax.axis_size(axis))
    return [values] + [swap(values, axis, mask) for mask in masks]


def paired_sum(parts):
    while len(parts) > 1:
        parts = [parts[i] + parts[i + 1] for i in range(0, len(parts), 2)]
    return parts[0]


def on_device(
    latent,
    condition,
    context,
    context_code,
    shift_weight,
    scale_weight,
    gate_weight,
    norm_gain,
    query_weight,
    key_weight,
    value_weight,
    output_weight,
    query_gain,
    key_gain,
    context_bias,
):
    head_dim = query_gain.shape[0]
    sp_size = lax.axis_size("sp")
    bf16, f32 = jnp.bfloat16, jnp.float32
    shape = jax.ShapeDtypeStruct
    latent, context = latent[0], context[0]
    seq_rows, width = latent.shape
    ctx_rows = context.shape[0]
    core = lax.axis_index("dp")
    index = jnp.stack([lax.axis_index("tp"), core]).astype(jnp.int32)
    gain_row, key_row, query_row = norm_gain[None], key_gain[None], query_gain[None]

    cols = shift_weight.shape[1]
    sources = [condition, context_code, shift_weight, scale_weight, gate_weight]
    partial_mod = call(
        modulation_kernel,
        pltpu.VMEM((8, cols), f32),
        [HBM] * 5,
        2**20,
        *(pltpu.with_memory_space_constraint(source, pltpu.HBM) for source in sources),
        scratch_shapes=[pltpu.VMEM(source.shape, bf16) for source in sources]
        + [pltpu.SemaphoreType.DMA((5,))],
    )
    blocks = sum(rows // math.gcd(rows, 64) for rows in (ctx_rows, seq_rows))
    context_tokens, latent_tokens, context_factor, latent_factor = call(
        normal_kernel,
        [
            pltpu.VMEM((ctx_rows, width), bf16),
            pltpu.VMEM((seq_rows, width), bf16),
            pltpu.VMEM((ctx_rows, 1), f32),
            pltpu.VMEM((seq_rows, 1), f32),
        ],
        [HBM] * 2,
        2**24,
        *(pltpu.with_memory_space_constraint(tokens, pltpu.HBM) for tokens in (context, latent)),
        scratch_shapes=[pltpu.SemaphoreType.DMA((blocks,))],
    )
    if direct(sp_size):
        summed = paired_sum(exchange(partial_mod, "sp"))
    else:
        summed = lax.psum(partial_mod, "sp")
    pieces = jnp.stack(exchange(summed, "tp"))

    near = core_swap(output_weight, "tp", (1, 2))
    half = output_weight.shape[0] // 2
    passed = lax.dynamic_slice_in_dim(near, core * half, half, 0)
    far = core_swap(passed, "tp", (2, 1))
    gathered = [near, far, swap(near, "dp", 1), swap(far, "dp", 1)]

    position = lax.axis_index("sp") * seq_rows + jnp.arange(seq_rows, dtype=jnp.int32)
    grid_row = (position // GRID_W).astype(f32)
    grid_col = (position % GRID_W).astype(f32)
    inverse = rope_base ** (-jnp.arange(head_dim // 4, dtype=f32) / (head_dim // 4))
    angles = jnp.concatenate([grid_row[:, None] * inverse, grid_col[:, None] * inverse], axis=-1)
    angles = jnp.concatenate([angles, angles], axis=-1)
    cosine, sine_part = jnp.cos(angles), jnp.sin(angles)

    own_kv, normed, gate_row = call(
        key_value_kernel,
        [
            shape((ctx_rows + seq_rows, 2 * head_dim), bf16),
            shape((seq_rows, width), bf16),
            shape((1, width), f32),
        ],
        [SMEM] + [VMEM] * 11,
        2**28,
        index,
        pieces,
        latent_tokens,
        context_tokens,
        latent_factor,
        context_factor,
        gain_row,
        key_weight.T,
        value_weight.T,
        key_row,
        cosine,
        sine_part,
        scratch_shapes=[pltpu.VMEM((8, width), f32)],
    )
    if direct(sp_size):
        pairs = exchange(own_kv, "sp")
    query_cols = query_weight.shape[1]
    heads = query_cols // head_dim
    score_scale = head_dim ** (-0.5)
    queries = call(
        functools.partial(query_kernel, score_scale),
        shape((heads * seq_rows, 2 * head_dim), bf16),
        [VMEM] * 5,
        2**28,
        normed,
        query_weight,
        query_row,
        cosine,
        sine_part,
    )
    if direct(sp_size):
        top_score, sums = call(
            functools.partial(attend_own_kernel, ctx_rows),
            [shape((heads * seq_rows, 1), f32), shape((heads * seq_rows, 2 * head_dim), f32)],
            [SMEM] + [VMEM] * 2,
            2**28,
            context_bias,
            queries,
            own_kv,
        )
        attended = call(
            functools.partial(attend_rest_kernel, ctx_rows),
            shape((seq_rows, query_cols), bf16),
            [SMEM] + [VMEM] * (2 + len(pairs)),
            2**30,
            context_bias,
            queries,
            top_score,
            sums,
            *pairs[1:],
        )
    else:
        attended = scanned_attention(own_kv, ctx_rows, queries, context_bias, head_dim, heads)

    heads_of = exchange(attended, "tp")
    own_partial = call(
        own_partial_kernel,
        shape((seq_rows, width), bf16),
        [VMEM] * 2,
        2**28,
        attended,
        output_weight,
    )
    block = math.gcd(width, 512)
    updated = pl.pallas_call(
        output_kernel,
        grid=(width // block,),
        out_shape=shape((seq_rows, width), bf16),
        in_specs=[SMEM] + [VMEM] * (6 + len(gathered)),
        out_specs=pl.BlockSpec((seq_rows, block), lambda i: (0, i)),
        cost_estimate=pl.CostEstimate(flops=2**30, bytes_accessed=0, transcendentals=0),
        name="output",
        compiler_params=pltpu.CompilerParams(vmem_limit_bytes=KERNEL_VMEM),
    )(index, own_partial, *heads_of[1:], latent, gate_row, *gathered)
    return updated[None]


def scanned_attention(own_kv, ctx_rows, queries, context_bias, head_dim, heads):
    contexts = lax.all_gather(own_kv[:ctx_rows], "sp", axis=0, tiled=True)
    arrived = lax.all_gather(own_kv[ctx_rows:], "sp", axis=0, tiled=True)
    query_rows = queries[:, :head_dim]
    seq_rows = query_rows.shape[0] // heads
    bias_rows = jnp.repeat(context_bias, seq_rows)
    scores = dot(query_rows, contexts[:, :head_dim].T) + bias_rows[:, None]
    first_max = scores.max(axis=1)
    weights = jnp.exp(scores - first_max[:, None])
    start = (
        first_max,
        weights.sum(axis=1),
        dot(weights.astype(jnp.bfloat16), contexts[:, head_dim:]),
    )
    block_rows = math.gcd(arrived.shape[0], 1024)
    blocks = arrived.reshape(-1, block_rows, 2 * head_dim)

    def absorb_block(state_now, pair_block):
        old_max, old_total, old_accum = state_now
        scores = dot(query_rows, pair_block[:, :head_dim].T)
        new_max = jnp.maximum(old_max, scores.max(axis=1))
        factor = jnp.exp(old_max - new_max)
        weights = jnp.exp(scores - new_max[:, None])
        new_accum = old_accum * factor[:, None] + dot(
            weights.astype(jnp.bfloat16), pair_block[:, head_dim:]
        )
        return ((new_max, old_total * factor + weights.sum(axis=1), new_accum), None)

    (row_max, totals, accum), unused = lax.scan(absorb_block, start, blocks)
    attended = (accum / totals[:, None]).astype(jnp.bfloat16)
    attended = attended.reshape(heads, seq_rows, head_dim).transpose(1, 0, 2)
    return attended.reshape(seq_rows, heads * head_dim)


def solution(mesh):
    return jax.shard_map(
        on_device,
        mesh=mesh,
        in_specs=(
            P("dp", "sp", None),
            P("dp", "sp"),
            P("dp", "sp", None),
            P("sp"),
            P("sp", "tp"),
            P("sp", "tp"),
            P("sp", "tp"),
            P(),
            P(None, "tp"),
            P(None, "tp"),
            P(None, "tp"),
            P("tp", None),
            P(),
            P(),
            P("tp"),
        ),
        out_specs=P("dp", "sp", None),
        check_vma=False,
    )
```
